32 devices in a mesh: fs: 8 (over z, y), tp: 4 (over x, core).
Axes of the slice: x: 2, y: 2, z: 4, core: 2. Of those that a mesh axis runs over, the one named last changes fastest.
Arguments:
- cotangent: bfloat16 [4096, 4096], P(('fs', 'tp')), may hold values from -6 to 6
- gate_pre: bfloat16 [4096, 6144], P('fs', 'tp'), may hold values from -8 to 8
- up_pre: bfloat16 [4096, 6144], P('fs', 'tp'), may hold values from -6 to 6
- down_weight: bfloat16 [4096, 6144], P('fs', 'tp'), may hold values from -0.078125 to 0.078125
Outputs:
- gate_grad: bfloat16 [4096, 6144], P('fs', 'tp')
- up_grad: bfloat16 [4096, 6144], P('fs', 'tp')
- down_grad: float32 [4096, 6144], P('fs', 'tp')
The draws below stay inside these ranges and needn't reach their ends.
All inputs are finite; a program needn't handle non-finite values.
Results may differ from the reference program's by a relative error of at most 0.0027.
Values may be sent and summed in bfloat16 or wider, within the bound.
A program may use at most 128 MiB of HBM per device.

```python
import math
import jax
import jax.numpy as jnp
from jax import lax

D = 4096
FF = 6144
TOKENS = 4096


def raised(array, rng, source, target, parts, factor):
    def block_of(dim):
        return (jnp.arange(array.shape[dim]) // (array.shape[dim] // parts)).reshape((-1,) + (1,) * (array.ndim - 1 - dim))

    first = jax.random.permutation(rng, parts)[block_of(target)]
    second = (block_of(target) + parts // 2) % parts
    return jnp.where((block_of(source) == first) | (block_of(source) == second), factor * array, array)


def block_scale(rng, dims, pieces, least, largest):
    gain = 1.0
    for axis_at, blocks in pieces:
        steps = jax.random.uniform(jax.random.fold_in(jax.random.fold_in(rng, 6), axis_at), (blocks,), jnp.float32, least / len(pieces), largest / len(pieces))
        gain = gain * jnp.repeat(jnp.exp(steps), dims[axis_at] // blocks).reshape((-1,) + (1,) * (len(dims) - 1 - axis_at))
    return gain


def noise(rng, shape, scale, most, cuts=(), kind=jnp.bfloat16):
    entries = jax.random.normal(rng, shape, jnp.float32) * scale
    if len(cuts) > 0:
        entries = block_scale(rng, shape, cuts, -0.22, 0.18) * entries
    return jnp.clip(entries, min=-most, max=most).astype(kind)


def gaussian_with(stream_key, dims, scale, limit, cuts, heavy, held_as=jnp.bfloat16):
    drawn = scale * jax.random.normal(stream_key, dims, jnp.float32)
    if cuts:
        drawn = drawn * block_scale(stream_key, dims, cuts, -0.22, 0.18)
    return jnp.clip(raised(drawn, jax.random.fold_in(stream_key, 3), *heavy), -limit, limit).astype(held_as)


def setup_inputs(seed: int = 0) -> dict:
    splits = jax.random.split(jax.random.key(seed), 5)
    cotangent = gaussian_with(splits[0], (TOKENS, D), 1.0, 6.0, ((0, 32),), (0, 1, 32, 2.75))
    gate_pre = noise(splits[1], (TOKENS, FF), 1.5, 8.0, ((0, 8), (1, 4)))
    up_pre = noise(splits[2], (TOKENS, FF), 1.0, 6.0, ((0, 8), (1, 4)))
    down_weight = noise(splits[3], (D, FF), FF ** -0.5, 0.078125, ((0, 8), (1, 4)))
    return dict(cotangent=cotangent, gate_pre=gate_pre, up_pre=up_pre, down_weight=down_weight)


def reference(cotangent, gate_pre, up_pre, down_weight):
    gate_values = gate_pre.astype(jnp.float32)
    up_values = up_pre.astype(jnp.float32)
    sigmoid_gate = jax.nn.sigmoid(gate_values)
    silu_gate = gate_values * sigmoid_gate
    hidden = (silu_gate * up_values).astype(jnp.bfloat16)
    hidden_grad = 0.5 * jnp.dot(cotangent, down_weight, preferred_element_type=jnp.float32)
    up_grad = (hidden_grad * silu_gate).astype(jnp.bfloat16)
    gate_grad = (hidden_grad * up_values * sigmoid_gate * (1.0 + gate_values * (1.0 - sigmoid_gate))).astype(jnp.bfloat16)
    product = lax.dot_general(cotangent, hidden, (((0,), (0,)), ((), ())), preferred_element_type=jnp.float32)
    down_grad = product * (0.5 / math.sqrt(TOKENS))
    return (gate_grad, up_grad, down_grad)
```

```python
import math

import jax
import jax.numpy as jnp
from jax import lax
from jax.sharding import PartitionSpec as P


def ring_moves(count):
    places = count // 2

    def shift(by):
        return [(2 * p + s, 2 * ((p + by) % places) + s) for p in range(places) for s in range(2)]

    swap = [(m, m ^ 1) for m in range(count)]
    return places, shift, swap


def distances(places):
    order = [0]
    for step in range(1, (places - 1) // 2 + 1):
        order += [-step, step]
    if places > 1 and places % 2 == 0:
        order.append(places // 2)
    return order


def ring_gather(block, places, shift):
    found = [block]
    from_left = from_right = block
    for _ in range((places - 1) // 2):
        from_left = lax.ppermute(from_left, "fs", shift(1))
        from_right = lax.ppermute(from_right, "fs", shift(-1))
        found += [from_left, from_right]
    if places > 1 and places % 2 == 0:
        half = block.shape[0] // 2
        found.append(
            jnp.concatenate(
                [
                    lax.ppermute(from_left[:half], "fs", shift(1)),
                    lax.ppermute(from_right[half:], "fs", shift(-1)),
                ]
            )
        )
    return jnp.concatenate(found)


def local(cotangent, gate_pre, up_pre, down_weight):
    count = lax.axis_size("fs")
    width = lax.axis_size("tp")
    rows = cotangent.shape[0]
    depth = down_weight.shape[0]
    grad_scale = 0.5 / math.sqrt(gate_pre.shape[0] * count)
    places, shift, swap = ring_moves(count)
    order = distances(places)
    me = lax.axis_index("fs")
    place, side = me // 2, me % 2

    def features(distance, which, many=1):
        member = 2 * ((place + distance + places) % places) + which
        return lax.dynamic_slice_in_dim(cotangent, member * depth, many * depth, axis=1)

    weights = ring_gather(down_weight, places, shift)

    mine = jnp.concatenate([features(d, side) for d in order], axis=1)
    theirs = jnp.concatenate([features(d, 1 - side) for d in order], axis=1)
    near = lax.all_gather(mine, "tp", axis=0, tiled=True)
    far = lax.all_gather(lax.ppermute(theirs, "fs", swap), "tp", axis=0, tiled=True)

    gate_values = gate_pre.astype(jnp.float32)
    up_values = up_pre.astype(jnp.float32)
    sigmoid_gate = jax.nn.sigmoid(gate_values)
    silu_gate = gate_values * sigmoid_gate
    hidden = (silu_gate * up_values).astype(jnp.bfloat16)
    hiddens = ring_gather(hidden, places, shift)

    pieces = []
    for d in order:
        piece = features(-d, 0, 2)
        pieces.append(piece if d == 0 else lax.ppermute(piece, "fs", shift(-d)))
    columns = lax.all_gather(jnp.stack(pieces), "tp", axis=1, tiled=True)
    columns = columns.reshape(places * width * rows, 2 * depth)

    far_part = jnp.dot(far, weights, preferred_element_type=jnp.float32)
    received = lax.ppermute(far_part, "fs", swap)
    contracted = jnp.dot(near, weights, preferred_element_type=jnp.float32) + received
    hidden_grad = 0.5 * contracted
    up_grad = (hidden_grad * silu_gate).astype(jnp.bfloat16)
    gate_grad = (
        hidden_grad * up_values * sigmoid_gate * (1.0 + gate_values * (1.0 - sigmoid_gate))
    ).astype(jnp.bfloat16)

    def share(which):
        part = lax.dynamic_slice_in_dim(columns, which * depth, depth, axis=1)
        return lax.dot_general(
            part, hiddens, (((0,), (0,)), ((), ())), preferred_element_type=jnp.float32
        )

    arrived = lax.ppermute(share(1 - side).astype(jnp.bfloat16), "fs", swap)
    down_grad = (share(side) + arrived.astype(jnp.float32)) * grad_scale
    return (gate_grad, up_grad, down_grad)


def solution(mesh):
    placed = (P(("fs", "tp"), None), P("fs", "tp"), P("fs", "tp"), P("fs", "tp"))
    return jax.shard_map(
        local,
        mesh=mesh,
        in_specs=placed,
        out_specs=(P("fs", "tp"), P("fs", "tp"), P("fs", "tp")),
        check_vma=False,
    )
```
